32 devices in a mesh: ep: 8 (over z, x), tp: 4 (over y, core).
Axes of the slice: x: 2, y: 2, z: 4, core: 2. Of those that a mesh axis runs over, the one named last changes fastest.
Arguments:
- tokens: bfloat16 [128, 1024], P('ep'), may hold values from -6 to 6
- norm_gain: float32 [1024], replicated, may hold values from 0.1 to 1.9
- routing: int32 [128, 2], P('ep'), may hold values from 0 to 7, all different within a row; in each aligned block of 16 rows (0 to 15, 16 to 31, ...) at most 8 rows name the same one
- route_weight: float32 [128, 2], P('ep'), may hold values from 0.1 to 1
- w_gate: bfloat16 [8, 1024, 3584], P('ep', None, 'tp'), may hold values from -0.1875 to 0.1875
- w_up: bfloat16 [8, 1024, 3584], P('ep', None, 'tp'), may hold values from -0.1875 to 0.1875
- w_down: bfloat16 [8, 3584, 1024], P('ep', 'tp'), may hold values from -0.09375 to 0.09375
Outputs:
- mixed: bfloat16 [128, 1024], P('ep', 'tp')
The draws below stay inside these ranges and needn't reach their ends.
Inputs may be any that keep to these rules, and one draw needn't show every extreme that they name: `routing`: each row names 2 different experts of 0 to 7; among the 16 tokens of one index of ep no expert is named more than 8 times, and in some draws' blocks exactly 8 times.
All inputs are finite; a program needn't handle non-finite values.
Results may differ from the reference program's by a relative error of at most 0.0022.
Values may be sent and summed in bfloat16 or wider, within the bound.
A program may use at most 64 MiB of HBM per device.

```python
import math
import jax
import jax.numpy as jnp
import numpy as np
from jax import lax

D = 1024
FF = 3584
TOP = 2
TOK_DEV = 16
CAP = 8
EXPERTS = 8
TOKENS = 128


def level_of(rng, shape, cuts, low, top_value):
    factor_of, own = 1.0, jax.random.fold_in(rng, 6)
    for position, shards_of in cuts:
        draws = jnp.exp(jax.random.uniform(jax.random.fold_in(own, position), (shards_of,), jnp.float32, low / len(cuts), top_value / len(cuts)))
        factor_of = factor_of * jnp.repeat(draws, shape[position] // shards_of).reshape([-1 if axis == position else 1 for axis in range(len(shape))])
    return factor_of


def shared_out(rng, own, number, rows, number_of, top, limit, lean):
    ranking = jax.random.permutation(rng, number_of)
    heavy_load, usual = portions_of(number_of, rows * top, limit, lean, True), portions_of(number_of, rows * top, limit, lean, False)
    places = jnp.arange(number_of)

    def named(sizes, rotation):
        used = int((sizes > 0).sum())
        fixed = max(1, used // 4)
        shifted = fixed + (places - fixed + rotation * (used - fixed)) % max(1, number_of - fixed)
        return jnp.zeros((number_of,), jnp.int32).at[ranking[jnp.where(places < fixed, places, shifted)]].set(jnp.asarray(sizes, jnp.int32))

    sizes = jnp.where(number % 4 == 0, named(heavy_load, number // 4), named(usual, number - number // 4 - 1))
    mixed = jax.random.permutation(jax.random.fold_in(own, 3), number_of)
    donor, taker = mixed[0:number_of // 2 * 2:2], mixed[1:number_of // 2 * 2:2]
    room = jnp.minimum(sizes[donor] - 1, limit - sizes[taker]) // 2
    room = jnp.where((donor == ranking[0]) | (taker == ranking[0]) | (sizes[taker] == 0), 0, jnp.maximum(room, 0))
    shifted = jax.random.randint(jax.random.fold_in(own, 4), (number_of // 2,), 0, 1 << 20) % (room + 1)
    sizes = sizes.at[donor].add(-shifted).at[taker].add(shifted)
    labels = jnp.searchsorted(jnp.cumsum(sizes), jnp.arange(rows * top), side="right").astype(jnp.int32)
    listing = labels.reshape(top, rows).T
    listing = listing[jax.random.permutation(jax.random.fold_in(own, 1), rows)]
    rotation = jax.random.randint(jax.random.fold_in(own, 2), (rows, 1), 0, top)
    return jnp.take_along_axis(listing, (jnp.arange(top)[None, :] + rotation) % top, axis=1)


def portions_of(count, total, most, slope, full):
    loads = [(1 << 20) // math.isqrt(grade ** slope) + 1 for grade in range(1, count + 1)]
    largest = most if full else min(most, max(-(-total // count), total * loads[0] // sum(loads)))
    least = 1 if total - largest >= count - 1 else 0
    counts, rest = [largest] + [least] * (count - 1), total - largest - least * (count - 1)
    while rest > 0:
        movable = [i for i in range(1, count) if counts[i] < largest] or [i for i in range(1, count) if counts[i] < most]
        whole, left = sum([loads[i] for i in movable]), rest
        for i in movable:
            extra = min(most - counts[i], max(1, left * loads[i] // whole), rest)
            counts[i] = counts[i] + extra
            rest = rest - extra
    return np.array(counts)


def scatter_about(own_key, dims, scale, reach, shards=(), kind=jnp.bfloat16):
    level = level_of(own_key, dims, shards, -0.22, 0.18) if shards else 1.0
    array = jax.random.normal(own_key, dims, jnp.float32) * scale * level
    return jnp.minimum(jnp.maximum(array, -reach), reach).astype(kind)


def setup_inputs(seed: int = 0) -> dict:
    seeds = jax.random.split(jax.random.key(seed), 8)
    tokens = scatter_about(seeds[0], (TOKENS, D), 1.0, 6.0, ((0, 8),))
    norm_gain = jnp.clip(1.0 + 0.18 * jax.random.normal(seeds[1], (D,), jnp.float32), 0.1, 1.9)
    routing_keys = jax.random.split(jax.random.fold_in(seeds[2], 1), TOKENS // TOK_DEV)
    routing_turns = jax.random.permutation(jax.random.fold_in(seeds[2], 3), TOKENS // TOK_DEV)
    routing = jax.vmap(lambda own, number: shared_out(jax.random.fold_in(seeds[2], 2), own, number, TOK_DEV, EXPERTS, TOP, CAP, 2))(routing_keys, routing_turns).reshape((TOKENS, TOP))
    route_weight = jnp.clip(0.1 + 0.9 * jax.random.uniform(seeds[3], (TOKENS, TOP), jnp.float32) ** level_of(seeds[3], (TOKENS, TOP), ((0, 8),), -0.2, 0.2), 0.1, 1.0)
    w_gate = scatter_about(seeds[4], (EXPERTS, D, FF), D ** -0.5, 0.1875, ((0, 8), (2, 4)))
    w_up = scatter_about(seeds[5], (EXPERTS, D, FF), D ** -0.5, 0.1875, ((0, 8), (2, 4)))
    w_down = scatter_about(seeds[6], (EXPERTS, FF, D), FF ** -0.5, 0.09375, ((0, 8), (1, 4)))
    return {"tokens": tokens, "norm_gain": norm_gain, "routing": routing, "route_weight": route_weight, "w_gate": w_gate, "w_up": w_up, "w_down": w_down}


norm_eps = 1e-06

def reference(tokens, norm_gain, routing, route_weight, w_gate, w_up, w_down):
    values = tokens.astype(jnp.float32)
    scale = lax.rsqrt(lax.optimization_barrier(jnp.mean(values * values, axis=-1, keepdims=True)) + norm_eps)
    normed = (values * scale * norm_gain).astype(jnp.bfloat16)
    top_count = routing.shape[1]
    flat_ids = routing.reshape(-1).astype(jnp.int32)
    token_rows = jnp.repeat(normed, top_count, axis=0)

    def one_slot(pair):
        token_row, expert_id = pair
        gate_act = jnp.dot(token_row[None, :], w_gate[expert_id], preferred_element_type=jnp.float32)
        up_act = jnp.dot(token_row[None, :], w_up[expert_id], preferred_element_type=jnp.float32)
        hidden = (jax.nn.silu(gate_act) * up_act).astype(jnp.bfloat16)
        return jnp.dot(hidden, w_down[expert_id], preferred_element_type=jnp.float32)[0]
    expert_out = lax.map(one_slot, (token_rows, flat_ids))
    expert_out = expert_out.reshape(routing.shape[0], top_count, -1)
    mixed = lax.optimization_barrier(jnp.sum(expert_out * route_weight[:, :, None], axis=1))
    return mixed.astype(jnp.bfloat16)
```

```python
import functools

import jax
import jax.numpy as jnp
from jax import lax
from jax.experimental import pallas as pl
from jax.experimental.pallas import tpu as pltpu
from jax.sharding import PartitionSpec as P

CAP = 8
MESH = pl.DeviceIdType.MESH

norm_eps = 1e-06


def each(low, high, step):
    if high - low <= 8:
        for index in range(low, high):
            step(index)
    else:
        lax.fori_loop(low, high, lambda index, carry: (step(index), carry)[1], 0)


def kernel(groups, shares, tokens, gain, routing, route_weight, gate_hbm, up_hbm, down_hbm, mixed,
           gate, up, down, outgoing, incoming, partial, arrived, load_sem, send_sem, recv_sem):
    ep, tp = lax.axis_index("ep"), lax.axis_index("tp")
    width = tokens.shape[1]
    part = mixed.shape[1]
    slots = groups * CAP
    cores = 2 if shares % 2 == 0 else 1
    rows = shares // cores

    def toward(q):
        return lax.rem(tp // cores + q // cores, rows) * cores + lax.rem(lax.rem(tp, cores) + q % cores, cores)

    loads = [pltpu.make_async_copy(source.at[0], target, load_sem.at[i])
             for i, (source, target) in enumerate(((gate_hbm, gate), (up_hbm, up), (down_hbm, down)))]
    for load in loads:
        load.start()

    barrier = pltpu.get_barrier_semaphore()
    for q in range(shares):
        peer = toward(q)

        def greet(d):
            pl.semaphore_signal(barrier, inc=1, device_id=(lax.rem(ep + d, groups), peer), device_id_type=MESH)
        each(1 if q == 0 else 0, groups, greet)

    values = tokens[...].astype(jnp.float32)
    scale = lax.rsqrt(jnp.mean(values * values, axis=-1, keepdims=True) + norm_eps)
    normed = (values * scale * gain[...]).astype(jnp.bfloat16)

    count = tokens.shape[0]
    lane = lax.broadcasted_iota(jnp.int32, (count, slots), 1)
    expert = lax.rem(lane // CAP + ep, groups)
    member = jnp.zeros((count, slots), jnp.float32)
    weight = jnp.zeros((count, slots), jnp.float32)
    for k in range(routing.shape[1]):
        named = routing[:, k:k + 1] == expert
        member = jnp.where(named, 1.0, member)
        weight = jnp.where(named, route_weight[:, k:k + 1], weight)
    earlier = lax.broadcasted_iota(jnp.int32, (count, count), 0) > lax.broadcasted_iota(jnp.int32, (count, count), 1)
    before = jnp.dot(jnp.where(earlier, 1.0, 0.0).astype(jnp.bfloat16), member.astype(jnp.bfloat16),
                     preferred_element_type=jnp.float32)
    placed = jnp.where(before == lax.rem(lane, CAP).astype(jnp.float32), member, 0.0)
    weight = weight * placed
    sent = lax.dot_general(placed.astype(jnp.bfloat16), normed, (((0,), (0,)), ((), ())),
                           preferred_element_type=jnp.float32)
    outgoing[...] = sent.reshape(groups, CAP, width).astype(jnp.bfloat16)

    pl.semaphore_wait(barrier, groups * shares - 1)

    def dispatch(d):
        pltpu.make_async_remote_copy(
            src_ref=outgoing.at[d], dst_ref=incoming.at[d], send_sem=send_sem.at[0], recv_sem=recv_sem.at[0],
            device_id=(lax.rem(ep + d, groups), tp), device_id_type=MESH).start()
    each(1, groups, dispatch)
    incoming[0] = outgoing[0]

    loads[0].wait()
    loads[1].wait()
    others = pl.ds(1, groups - 1)
    pltpu.make_async_copy(incoming.at[others], incoming.at[others], recv_sem.at[0]).wait()

    x = incoming[...].astype(jnp.float32).reshape(slots, width).astype(jnp.bfloat16)
    gate_act = jnp.dot(x, gate[...], preferred_element_type=jnp.float32)
    up_act = jnp.dot(x, up[...], preferred_element_type=jnp.float32)
    hidden = (gate_act / (1.0 + jnp.exp(-gate_act)) * up_act).astype(jnp.bfloat16)
    loads[2].wait()

    for q in reversed(range(shares)):
        peer = toward(q)
        columns = pl.ds(pl.multiple_of(peer * part, part), part)
        block = jnp.dot(hidden, down[:, columns], preferred_element_type=jnp.float32)
        partial[q * groups:(q + 1) * groups] = block.reshape(groups, CAP, part)

        def give(d):
            pltpu.make_async_remote_copy(
                src_ref=partial.at[q * groups + d], dst_ref=arrived.at[q * groups + d],
                send_sem=send_sem.at[1], recv_sem=recv_sem.at[1],
                device_id=(lax.rem(ep - d + groups, groups), peer), device_id_type=MESH).start()
        each(1 if q == 0 else 0, groups, give)
    arrived[0] = partial[0]

    rest = pl.ds(1, groups * shares - 1)
    pltpu.make_async_copy(arrived.at[rest], arrived.at[rest], recv_sem.at[1]).wait()
    total = arrived[0:groups]
    for q in range(1, shares):
        total = total + arrived[q * groups:(q + 1) * groups]
    out = jnp.dot(weight, total.reshape(slots, part), precision=lax.Precision.HIGHEST,
                  preferred_element_type=jnp.float32)
    mixed[...] = out.astype(mixed.dtype)
    pltpu.make_async_copy(outgoing.at[others], outgoing.at[others], send_sem.at[0]).wait()
    pltpu.make_async_copy(partial.at[rest], partial.at[rest], send_sem.at[1]).wait()


def solution(mesh):
    groups, shares = mesh.shape["ep"], mesh.shape["tp"]

    def local(tokens, norm_gain, routing, route_weight, w_gate, w_up, w_down):
        count, width = tokens.shape
        part = width // shares
        vmem = pl.BlockSpec(memory_space=pltpu.VMEM)
        hbm = pl.BlockSpec(memory_space=pltpu.HBM)
        return pl.pallas_call(
            functools.partial(kernel, groups, shares),
            out_shape=jax.ShapeDtypeStruct((count, part), jnp.bfloat16),
            in_specs=[vmem] * 4 + [hbm] * 3,
            out_specs=vmem,
            scratch_shapes=[
                pltpu.VMEM(w_gate.shape[1:], jnp.bfloat16),
                pltpu.VMEM(w_up.shape[1:], jnp.bfloat16),
                pltpu.VMEM(w_down.shape[1:], jnp.bfloat16),
                pltpu.VMEM((groups, CAP, width), jnp.bfloat16),
                pltpu.VMEM((groups, CAP, width), jnp.bfloat16),
                pltpu.VMEM((groups * shares, CAP, part), jnp.float32),
                pltpu.VMEM((groups * shares, CAP, part), jnp.float32),
                pltpu.SemaphoreType.DMA((3,)),
                pltpu.SemaphoreType.DMA((2,)),
                pltpu.SemaphoreType.DMA((2,)),
            ],
            compiler_params=pltpu.CompilerParams(collective_id=0, has_side_effects=True,
                                                 vmem_limit_bytes=40 * 1024 * 1024),
            name="experts",
        )(tokens, norm_gain.reshape(1, width), routing, route_weight, w_gate, w_up, w_down)

    in_specs = (
        P("ep", None),
        P(),
        P("ep", None),
        P("ep", None),
        P("ep", None, "tp"),
        P("ep", None, "tp"),
        P("ep", "tp", None),
    )
    return jax.shard_map(local, mesh=mesh, in_specs=in_specs, out_specs=P("ep", "tp"), check_vma=False)
```

```python
import functools

import jax
import jax.numpy as jnp
from jax import lax
from jax.experimental import pallas as pl
from jax.experimental.pallas import tpu as pltpu
from jax.sharding import PartitionSpec as P

CAP = 8
MESH = pl.DeviceIdType.MESH

norm_eps = 1e-06


def each(low, high, step):
    if high - low <= 8:
        for index in range(low, high):
            step(index)
    else:
        lax.fori_loop(low, high, lambda index, carry: (step(index), carry)[1], 0)


def kernel(groups, shares, tokens_hbm, gain_hbm, routing_hbm, route_weight_hbm, gate_hbm, up_hbm, down_hbm, mixed,
           tokens, gain, routing, route_weight,
           gate, up, down, outgoing, incoming, partial, arrived, load_sem, send_sem, recv_sem):
    ep, tp = lax.axis_index("ep"), lax.axis_index("tp")
    width = tokens.shape[1]
    part = mixed.shape[1]
    slots = groups * CAP
    cores = 2 if shares % 2 == 0 else 1
    rows = shares // cores

    def toward(q):
        return lax.rem(tp // cores + q // cores, rows) * cores + lax.rem(lax.rem(tp, cores) + q % cores, cores)

    pairs = ((tokens_hbm, tokens), (gain_hbm, gain), (routing_hbm, routing), (route_weight_hbm, route_weight),
             (gate_hbm.at[0], gate), (up_hbm.at[0], up), (down_hbm.at[0], down))
    loads = [pltpu.make_async_copy(source, target, load_sem.at[i]) for i, (source, target) in enumerate(pairs)]
    for load in loads:
        load.start()

    barrier = pltpu.get_barrier_semaphore()

    def greet(d):
        pl.semaphore_signal(barrier, inc=1, device_id=(lax.rem(ep + d, groups), tp), device_id_type=MESH)
    each(1, groups, greet)
    for q in range(1, shares):
        pl.semaphore_signal(barrier, inc=1, device_id=(ep, toward(q)), device_id_type=MESH)

    count = tokens.shape[0]
    line = lax.broadcasted_iota(jnp.int32, (slots, count), 0)
    expert = lax.rem(line // CAP + ep, groups)
    member = jnp.zeros((slots, count), jnp.float32)
    weight = jnp.zeros((slots, count), jnp.float32)
    loads[2].wait()
    loads[3].wait()
    for k in range(routing.shape[0]):
        named = routing[k:k + 1, :] == expert
        member = jnp.where(named, 1.0, member)
        weight = jnp.where(named, route_weight[k:k + 1, :], weight)
    earlier = lax.broadcasted_iota(jnp.int32, (count, count), 0) < lax.broadcasted_iota(jnp.int32, (count, count), 1)
    before = jnp.dot(member.astype(jnp.bfloat16), jnp.where(earlier, 1.0, 0.0).astype(jnp.bfloat16),
                     preferred_element_type=jnp.float32)
    placed = jnp.where(before == lax.rem(line, CAP).astype(jnp.float32), member, 0.0)
    weight = jnp.transpose(weight * placed)

    loads[0].wait()
    loads[1].wait()
    values = tokens[...].astype(jnp.float32)
    scale = lax.rsqrt(jnp.mean(values * values, axis=-1, keepdims=True) + norm_eps)
    normed = (values * scale * gain[...]).astype(jnp.bfloat16)
    sent = jnp.dot(placed.astype(jnp.bfloat16), normed, preferred_element_type=jnp.float32)
    outgoing[...] = sent.reshape(groups, CAP, width).astype(jnp.bfloat16)

    pl.semaphore_wait(barrier, groups + shares - 2)

    def dispatch(d):
        pltpu.make_async_remote_copy(
            src_ref=outgoing.at[d], dst_ref=incoming.at[d], send_sem=send_sem.at[0], recv_sem=recv_sem.at[0],
            device_id=(lax.rem(ep + d, groups), tp), device_id_type=MESH).start()
    each(1, groups, dispatch)
    incoming[0] = outgoing[0]

    loads[4].wait()
    loads[5].wait()
    others = pl.ds(1, groups - 1)
    pltpu.make_async_copy(incoming.at[others], incoming.at[others], recv_sem.at[0]).wait()

    x = incoming[...].astype(jnp.float32).reshape(slots, width).astype(jnp.bfloat16)
    gate_act = jnp.dot(x, gate[...], preferred_element_type=jnp.float32)
    up_act = jnp.dot(x, up[...], preferred_element_type=jnp.float32)
    hidden = (gate_act / (1.0 + jnp.exp(-gate_act)) * up_act).astype(jnp.bfloat16)
    loads[6].wait()

    for q in reversed(range(shares)):
        peer = toward(q)
        columns = pl.ds(pl.multiple_of(peer * part, part), part)
        block = jnp.dot(hidden, down[:, columns], preferred_element_type=jnp.float32)
        partial[q * groups:(q + 1) * groups] = block.reshape(groups, CAP, part)

        def give(d):
            pltpu.make_async_remote_copy(
                src_ref=partial.at[q * groups + d], dst_ref=arrived.at[q * groups + d],
                send_sem=send_sem.at[1], recv_sem=recv_sem.at[1],
                device_id=(lax.rem(ep - d + groups, groups), peer), device_id_type=MESH).start()
        each(1 if q == 0 else 0, groups, give)
    arrived[0] = partial[0]

    rest = pl.ds(1, groups * shares - 1)
    pltpu.make_async_copy(arrived.at[rest], arrived.at[rest], recv_sem.at[1]).wait()
    total = arrived[0:groups]
    for q in range(1, shares):
        total = total + arrived[q * groups:(q + 1) * groups]
    out = jnp.dot(weight, total.reshape(slots, part), precision=lax.Precision.HIGHEST,
                  preferred_element_type=jnp.float32)
    mixed[...] = out.astype(mixed.dtype)
    pltpu.make_async_copy(outgoing.at[others], outgoing.at[others], send_sem.at[0]).wait()
    pltpu.make_async_copy(partial.at[rest], partial.at[rest], send_sem.at[1]).wait()


def solution(mesh):
    groups, shares = mesh.shape["ep"], mesh.shape["tp"]

    def local(tokens, norm_gain, routing, route_weight, w_gate, w_up, w_down):
        count, width = tokens.shape
        part = width // shares
        vmem = pl.BlockSpec(memory_space=pltpu.VMEM)
        hbm = pl.BlockSpec(memory_space=pltpu.HBM)
        return pl.pallas_call(
            functools.partial(kernel, groups, shares),
            out_shape=jax.ShapeDtypeStruct((count, part), jnp.bfloat16),
            in_specs=[hbm] * 7,
            out_specs=vmem,
            scratch_shapes=[
                pltpu.VMEM((count, width), tokens.dtype),
                pltpu.VMEM((1, width), norm_gain.dtype),
                pltpu.VMEM(routing.shape[::-1], routing.dtype),
                pltpu.VMEM(route_weight.shape[::-1], route_weight.dtype),
                pltpu.VMEM(w_gate.shape[1:], jnp.bfloat16),
                pltpu.VMEM(w_up.shape[1:], jnp.bfloat16),
                pltpu.VMEM(w_down.shape[1:], jnp.bfloat16),
                pltpu.VMEM((groups, CAP, width), jnp.bfloat16),
                pltpu.VMEM((groups, CAP, width), jnp.bfloat16),
                pltpu.VMEM((groups * shares, CAP, part), jnp.float32),
                pltpu.VMEM((groups * shares, CAP, part), jnp.float32),
                pltpu.SemaphoreType.DMA((7,)),
                pltpu.SemaphoreType.DMA((2,)),
                pltpu.SemaphoreType.DMA((2,)),
            ],
            compiler_params=pltpu.CompilerParams(collective_id=0, has_side_effects=True,
                                                 vmem_limit_bytes=67043328),
            name="experts",
        )(tokens, norm_gain.reshape(1, width), routing.T, route_weight.T, w_gate, w_up, w_down)

    in_specs = (
        P("ep", None),
        P(),
        P("ep", None),
        P("ep", None),
        P("ep", None, "tp"),
        P("ep", None, "tp"),
        P("ep", "tp", None),
    )
    return jax.shard_map(local, mesh=mesh, in_specs=in_specs, out_specs=P("ep", "tp"), check_vma=False)
```

```python
import functools

import jax
import jax.numpy as jnp
from jax import lax
from jax.experimental import pallas as pl
from jax.experimental.pallas import tpu as pltpu
from jax.sharding import PartitionSpec as P

CAP = 8
MESH = pl.DeviceIdType.MESH

norm_eps = 1e-06


def each(low, high, step):
    if high - low <= 8:
        for index in range(low, high):
            step(index)
    else:
        lax.fori_loop(low, high, lambda index, carry: (step(index), carry)[1], 0)


def kernel(groups, shares, tokens_hbm, gain_hbm, routing_hbm, route_weight_hbm, gate_hbm, up_hbm, down_hbm, mixed,
           tokens, gain, routing, route_weight,
           gate, up, down, outgoing, incoming, lent, borrowed, partial, arrived, load_sem, send_sem, recv_sem):
    ep, tp = lax.axis_index("ep"), lax.axis_index("tp")
    width = tokens.shape[1]
    part = mixed.shape[1]
    slots = groups * CAP
    rows = shares // 2
    row, core = tp // 2, lax.rem(tp, 2)

    def toward(q):
        return lax.rem(row + q // 2, rows) * 2 + lax.rem(core + q % 2, 2)

    pairs = ((tokens_hbm, tokens), (gain_hbm, gain), (routing_hbm, routing), (route_weight_hbm, route_weight),
             (gate_hbm.at[0], gate), (up_hbm.at[0], up), (down_hbm.at[0], down))
    loads = [pltpu.make_async_copy(source, target, load_sem.at[i]) for i, (source, target) in enumerate(pairs)]
    for load in loads:
        load.start()

    barrier = pltpu.get_barrier_semaphore()

    def greet(d):
        pl.semaphore_signal(barrier, inc=1, device_id=(lax.rem(ep + d, groups), tp), device_id_type=MESH)
    each(1, groups, greet)
    for q in [1] + [2 * q for q in range(1, rows)]:
        pl.semaphore_signal(barrier, inc=1, device_id=(ep, toward(q)), device_id_type=MESH)

    count = tokens.shape[0]
    line = lax.broadcasted_iota(jnp.int32, (slots, count), 0)
    expert = lax.rem(line // CAP + ep, groups)
    member = jnp.zeros((slots, count), jnp.float32)
    weight = jnp.zeros((slots, count), jnp.float32)
    loads[2].wait()
    loads[3].wait()
    for k in range(routing.shape[0]):
        named = routing[k:k + 1, :] == expert
        member = jnp.where(named, 1.0, member)
        weight = jnp.where(named, route_weight[k:k + 1, :], weight)
    earlier = lax.broadcasted_iota(jnp.int32, (count, count), 0) < lax.broadcasted_iota(jnp.int32, (count, count), 1)
    before = jnp.dot(member.astype(jnp.bfloat16), jnp.where(earlier, 1.0, 0.0).astype(jnp.bfloat16),
                     preferred_element_type=jnp.float32)
    placed = jnp.where(before == lax.rem(line, CAP).astype(jnp.float32), member, 0.0)
    weight = jnp.transpose(weight * placed)

    loads[0].wait()
    loads[1].wait()
    values = tokens[...].astype(jnp.float32)
    scale = lax.rsqrt(jnp.mean(values * values, axis=-1, keepdims=True) + norm_eps)
    normed = (values * scale * gain[...]).astype(jnp.bfloat16)
    sent = jnp.dot(placed.astype(jnp.bfloat16), normed, preferred_element_type=jnp.float32)
    outgoing[...] = sent.reshape(groups, CAP, width).astype(jnp.bfloat16)

    pl.semaphore_wait(barrier, groups + rows - 1)

    def dispatch(d):
        pltpu.make_async_remote_copy(
            src_ref=outgoing.at[d], dst_ref=incoming.at[d], send_sem=send_sem.at[0], recv_sem=recv_sem.at[0],
            device_id=(lax.rem(ep + d, groups), tp), device_id_type=MESH).start()
    each(1, groups, dispatch)
    incoming[0] = outgoing[0]

    loads[4].wait()
    loads[5].wait()
    others = pl.ds(1, groups - 1)
    pltpu.make_async_copy(incoming.at[others], incoming.at[others], recv_sem.at[0]).wait()

    x = incoming[...].astype(jnp.float32).reshape(slots, width).astype(jnp.bfloat16)
    gate_act = jnp.dot(x, gate[...], preferred_element_type=jnp.float32)
    up_act = jnp.dot(x, up[...], preferred_element_type=jnp.float32)
    hidden = (gate_act / (1.0 + jnp.exp(-gate_act)) * up_act).astype(jnp.bfloat16)
    loads[6].wait()

    def block_of(q, side):
        columns = pl.ds(pl.multiple_of((lax.rem(row + q, rows) * 2 + side) * part, part), part)
        return jnp.dot(hidden, down[:, columns], preferred_element_type=jnp.float32)

    lends = []
    for q in reversed(range(rows)):
        lent[q] = block_of(q, 1 - core)
        lends.append(pltpu.make_async_remote_copy(
            src_ref=lent.at[q], dst_ref=borrowed.at[q], send_sem=send_sem.at[2 + q], recv_sem=recv_sem.at[2 + q],
            device_id=(ep, row * 2 + 1 - core), device_id_type=MESH))
        lends[-1].start()

    for q, lend in zip(reversed(range(rows)), lends):
        block = block_of(q, core)
        lend.wait_recv()
        partial[q * groups:(q + 1) * groups] = (block + borrowed[q]).reshape(groups, CAP, part)

        def give(d):
            pltpu.make_async_remote_copy(
                src_ref=partial.at[q * groups + d], dst_ref=arrived.at[q * groups + d],
                send_sem=send_sem.at[1], recv_sem=recv_sem.at[1],
                device_id=(lax.rem(ep - d + groups, groups), toward(2 * q)), device_id_type=MESH).start()
        each(1 if q == 0 else 0, groups, give)
    arrived[0] = partial[0]

    rest = pl.ds(1, groups * rows - 1)
    pltpu.make_async_copy(arrived.at[rest], arrived.at[rest], recv_sem.at[1]).wait()
    total = arrived[0:groups]
    for q in range(1, rows):
        total = total + arrived[q * groups:(q + 1) * groups]
    out = jnp.dot(weight, total.reshape(slots, part), precision=lax.Precision.HIGHEST,
                  preferred_element_type=jnp.float32)
    mixed[...] = out.astype(mixed.dtype)
    pltpu.make_async_copy(outgoing.at[others], outgoing.at[others], send_sem.at[0]).wait()
    pltpu.make_async_copy(partial.at[rest], partial.at[rest], send_sem.at[1]).wait()
    for lend in lends:
        lend.wait_send()


def solution(mesh):
    groups, shares = mesh.shape["ep"], mesh.shape["tp"]

    def local(tokens, norm_gain, routing, route_weight, w_gate, w_up, w_down):
        count, width = tokens.shape
        part = width // shares
        vmem = pl.BlockSpec(memory_space=pltpu.VMEM)
        hbm = pl.BlockSpec(memory_space=pltpu.HBM)
        return pl.pallas_call(
            functools.partial(kernel, groups, shares),
            out_shape=jax.ShapeDtypeStruct((count, part), jnp.bfloat16),
            in_specs=[hbm] * 7,
            out_specs=vmem,
            scratch_shapes=[
                pltpu.VMEM((count, width), tokens.dtype),
                pltpu.VMEM((1, width), norm_gain.dtype),
                pltpu.VMEM(routing.shape[::-1], routing.dtype),
                pltpu.VMEM(route_weight.shape[::-1], route_weight.dtype),
                pltpu.VMEM(w_gate.shape[1:], jnp.bfloat16),
                pltpu.VMEM(w_up.shape[1:], jnp.bfloat16),
                pltpu.VMEM(w_down.shape[1:], jnp.bfloat16),
                pltpu.VMEM((groups, CAP, width), jnp.bfloat16),
                pltpu.VMEM((groups, CAP, width), jnp.bfloat16),
                pltpu.VMEM((shares // 2, groups * CAP, part), jnp.float32),
                pltpu.VMEM((shares // 2, groups * CAP, part), jnp.float32),
                pltpu.VMEM((groups * shares // 2, CAP, part), jnp.float32),
                pltpu.VMEM((groups * shares // 2, CAP, part), jnp.float32),
                pltpu.SemaphoreType.DMA((7,)),
                pltpu.SemaphoreType.DMA((2 + shares // 2,)),
                pltpu.SemaphoreType.DMA((2 + shares // 2,)),
            ],
            compiler_params=pltpu.CompilerParams(collective_id=0, has_side_effects=True,
                                                 vmem_limit_bytes=67043328 - 16384),
            name="experts",
        )(tokens, norm_gain.reshape(1, width), routing.T, route_weight.T, w_gate, w_up, w_down)

    in_specs = (
        P("ep", None),
        P(),
        P("ep", None),
        P("ep", None),
        P("ep", None, "tp"),
        P("ep", None, "tp"),
        P("ep", "tp", None),
    )
    return jax.shard_map(local, mesh=mesh, in_specs=in_specs, out_specs=P("ep", "tp"), check_vma=False)
```

```python
import functools

import jax
import jax.numpy as jnp
from jax import lax
from jax.experimental import pallas as pl
from jax.experimental.pallas import tpu as pltpu
from jax.sharding import PartitionSpec as P

CAP = 8
MESH = pl.DeviceIdType.MESH

norm_eps = 1e-06


def each(low, high, step):
    if high - low <= 8:
        for index in range(low, high):
            step(index)
    else:
        lax.fori_loop(low, high, lambda index, carry: (step(index), carry)[1], 0)


def kernel(groups, shares, tokens_hbm, gain_hbm, routing_hbm, route_weight_hbm, gate_hbm, up_hbm, down_hbm, mixed,
           tokens, gain, routing, route_weight,
           gate, up, down, outgoing, incoming, lent, borrowed, partial, arrived, load_sem, send_sem, recv_sem):
    ep, tp = lax.axis_index("ep"), lax.axis_index("tp")
    width = tokens.shape[1]
    part = mixed.shape[1]
    slots = groups * CAP
    rows = shares // 2
    row, core = tp // 2, lax.rem(tp, 2)

    def toward(q):
        return lax.rem(row + q // 2, rows) * 2 + lax.rem(core + q % 2, 2)

    def far_first(step):
        return step + (1 - 2 * ep // groups) * (groups - 1 - 2 * step)

    pairs = ((tokens_hbm, tokens), (gain_hbm, gain), (routing_hbm, routing), (route_weight_hbm, route_weight),
             (gate_hbm.at[0], gate), (up_hbm.at[0], up), (down_hbm.at[0], down))
    loads = [pltpu.make_async_copy(source, target, load_sem.at[i]) for i, (source, target) in enumerate(pairs)]
    for load in loads:
        load.start()

    barrier = pltpu.get_barrier_semaphore()

    def greet(d):
        pl.semaphore_signal(barrier, inc=1, device_id=(lax.rem(ep + d, groups), tp), device_id_type=MESH)
    each(1, groups, greet)
    for q in range(1, shares):
        pl.semaphore_signal(barrier, inc=1, device_id=(ep, toward(q)), device_id_type=MESH)

    count = tokens.shape[0]
    line = lax.broadcasted_iota(jnp.int32, (slots, count), 0)
    expert = lax.rem(line // CAP + ep, groups)
    member = jnp.zeros((slots, count), jnp.float32)
    weight = jnp.zeros((slots, count), jnp.float32)
    loads[2].wait()
    loads[3].wait()
    for k in range(routing.shape[0]):
        named = routing[k:k + 1, :] == expert
        member = jnp.where(named, 1.0, member)
        weight = jnp.where(named, route_weight[k:k + 1, :], weight)
    earlier = lax.broadcasted_iota(jnp.int32, (count, count), 0) < lax.broadcasted_iota(jnp.int32, (count, count), 1)
    before = jnp.dot(member.astype(jnp.bfloat16), jnp.where(earlier, 1.0, 0.0).astype(jnp.bfloat16),
                     preferred_element_type=jnp.float32)
    placed = jnp.where(before == lax.rem(line, CAP).astype(jnp.float32), member, 0.0)
    weight = jnp.transpose(weight * placed)

    loads[0].wait()
    loads[1].wait()
    values = tokens[...].astype(jnp.float32)
    scale = lax.rsqrt(jnp.mean(values * values, axis=-1, keepdims=True) + norm_eps)
    normed = (values * scale * gain[...]).astype(jnp.bfloat16)
    sent = jnp.dot(placed.astype(jnp.bfloat16), normed, preferred_element_type=jnp.float32)
    outgoing[...] = sent.reshape(groups, CAP, width).astype(jnp.bfloat16)

    pl.semaphore_wait(barrier, groups + shares - 2)

    def dispatch(d):
        pltpu.make_async_remote_copy(
            src_ref=outgoing.at[d], dst_ref=incoming.at[d], send_sem=send_sem.at[0], recv_sem=recv_sem.at[0],
            device_id=(lax.rem(ep + d, groups), tp), device_id_type=MESH).start()
    each(1, groups, dispatch)
    incoming[0] = outgoing[0]

    loads[4].wait()
    loads[5].wait()
    others = pl.ds(1, groups - 1)
    pltpu.make_async_copy(incoming.at[others], incoming.at[others], recv_sem.at[0]).wait()

    x = incoming[...].astype(jnp.float32).reshape(slots, width).astype(jnp.bfloat16)
    gate_act = jnp.dot(x, gate[...], preferred_element_type=jnp.float32)
    up_act = jnp.dot(x, up[...], preferred_element_type=jnp.float32)
    hidden = (gate_act / (1.0 + jnp.exp(-gate_act)) * up_act).astype(jnp.bfloat16)
    loads[6].wait()

    def block_of(q, side):
        columns = pl.ds(pl.multiple_of((lax.rem(row + q, rows) * 2 + side) * part, part), part)
        return jnp.dot(hidden, down[:, columns], preferred_element_type=jnp.float32)

    def give(place, q):
        def to(step):
            target = far_first(step)

            def copy():
                d = lax.rem(ep - target + groups, groups)
                pltpu.make_async_remote_copy(
                    src_ref=partial.at[place * groups + d], dst_ref=arrived.at[place * groups + d],
                    send_sem=send_sem.at[1], recv_sem=recv_sem.at[1],
                    device_id=(target, toward(q)), device_id_type=MESH).start()
            if q == 0:
                pl.when(target != ep)(copy)
            else:
                copy()
        each(0, groups, to)

    for q in range(2, shares):
        block = block_of(q // 2, lax.rem(core + q, 2))
        partial[(q - 1) * groups:q * groups] = block.reshape(groups, CAP, part)
        give(q - 1, q)

    lent[...] = block_of(0, 1 - core)
    lend = pltpu.make_async_remote_copy(
        src_ref=lent, dst_ref=borrowed, send_sem=send_sem.at[2], recv_sem=recv_sem.at[2],
        device_id=(ep, toward(1)), device_id_type=MESH)
    lend.start()
    block = block_of(0, core)
    lend.wait_recv()
    partial[0:groups] = (block + borrowed[...]).reshape(groups, CAP, part)
    give(0, 0)
    arrived[0] = partial[0]

    rest = pl.ds(1, groups * (shares - 1) - 1)
    pltpu.make_async_copy(arrived.at[rest], arrived.at[rest], recv_sem.at[1]).wait()
    total = arrived[0:groups]
    for q in range(1, shares - 1):
        total = total + arrived[q * groups:(q + 1) * groups]
    out = jnp.dot(weight, total.reshape(slots, part), precision=lax.Precision.HIGHEST,
                  preferred_element_type=jnp.float32)
    mixed[...] = out.astype(mixed.dtype)
    pltpu.make_async_copy(outgoing.at[others], outgoing.at[others], send_sem.at[0]).wait()
    pltpu.make_async_copy(partial.at[rest], partial.at[rest], send_sem.at[1]).wait()
    lend.wait_send()


def solution(mesh):
    groups, shares = mesh.shape["ep"], mesh.shape["tp"]

    def local(tokens, norm_gain, routing, route_weight, w_gate, w_up, w_down):
        count, width = tokens.shape
        part = width // shares
        vmem = pl.BlockSpec(memory_space=pltpu.VMEM)
        hbm = pl.BlockSpec(memory_space=pltpu.HBM)
        return pl.pallas_call(
            functools.partial(kernel, groups, shares),
            out_shape=jax.ShapeDtypeStruct((count, part), jnp.bfloat16),
            in_specs=[hbm] * 7,
            out_specs=vmem,
            scratch_shapes=[
                pltpu.VMEM((count, width), tokens.dtype),
                pltpu.VMEM((1, width), norm_gain.dtype),
                pltpu.VMEM(routing.shape[::-1], routing.dtype),
                pltpu.VMEM(route_weight.shape[::-1], route_weight.dtype),
                pltpu.VMEM(w_gate.shape[1:], jnp.bfloat16),
                pltpu.VMEM(w_up.shape[1:], jnp.bfloat16),
                pltpu.VMEM(w_down.shape[1:], jnp.bfloat16),
                pltpu.VMEM((groups, CAP, width), jnp.bfloat16),
                pltpu.VMEM((groups, CAP, width), jnp.bfloat16),
                pltpu.VMEM((groups * CAP, part), jnp.float32),
                pltpu.VMEM((groups * CAP, part), jnp.float32),
                pltpu.VMEM((groups * (shares - 1), CAP, part), jnp.float32),
                pltpu.VMEM((groups * (shares - 1), CAP, part), jnp.float32),
                pltpu.SemaphoreType.DMA((7,)),
                pltpu.SemaphoreType.DMA((3,)),
                pltpu.SemaphoreType.DMA((3,)),
            ],
            compiler_params=pltpu.CompilerParams(collective_id=0, has_side_effects=True,
                                                 vmem_limit_bytes=67043328),
            name="experts",
        )(tokens, norm_gain.reshape(1, width), routing.T, route_weight.T, w_gate, w_up, w_down)

    in_specs = (
        P("ep", None),
        P(),
        P("ep", None),
        P("ep", None),
        P("ep", None, "tp"),
        P("ep", None, "tp"),
        P("ep", "tp", None),
    )
    return jax.shard_map(local, mesh=mesh, in_specs=in_specs, out_specs=P("ep", "tp"), check_vma=False)
```

```python
import functools

import jax
import jax.numpy as jnp
from jax import lax
from jax.experimental import pallas as pl
from jax.experimental.pallas import tpu as pltpu
from jax.sharding import PartitionSpec as P

CAP = 8
MESH = pl.DeviceIdType.MESH

norm_eps = 1e-06


def each(low, high, step):
    if high - low <= 8:
        for index in range(low, high):
            step(index)
    else:
        lax.fori_loop(low, high, lambda index, carry: (step(index), carry)[1], 0)


def kernel(groups, shares, tokens_hbm, gain_hbm, routing_hbm, route_weight_hbm, gate_hbm, up_hbm, down_hbm, mixed,
           tokens, gain, routing, route_weight,
           gate, up, down, outgoing, incoming, lent, borrowed, partial, arrived, load_sem, send_sem, recv_sem):
    ep, tp = lax.axis_index("ep"), lax.axis_index("tp")
    width = tokens.shape[1]
    part = mixed.shape[1]
    slots = groups * CAP
    rows = shares // 2
    row, core = tp // 2, lax.rem(tp, 2)

    def toward(q):
        return lax.rem(row + q // 2, rows) * 2 + lax.rem(core + q % 2, 2)

    def far_first(step):
        return step + (1 - 2 * ep // groups) * (groups - 1 - 2 * step)

    pairs = ((tokens_hbm, tokens), (gain_hbm, gain), (routing_hbm, routing), (route_weight_hbm, route_weight),
             (gate_hbm.at[0], gate), (up_hbm.at[0], up), (down_hbm.at[0], down))
    loads = [pltpu.make_async_copy(source, target, load_sem.at[i]) for i, (source, target) in enumerate(pairs)]
    for load in loads:
        load.start()

    barrier = pltpu.get_barrier_semaphore()

    def greet(d):
        pl.semaphore_signal(barrier, inc=1, device_id=(lax.rem(ep + d, groups), tp), device_id_type=MESH)
    each(1, groups, greet)
    for q in range(1, shares):
        pl.semaphore_signal(barrier, inc=1, device_id=(ep, toward(q)), device_id_type=MESH)

    count = tokens.shape[0]
    line = lax.broadcasted_iota(jnp.int32, (slots, count), 0)
    expert = lax.rem(line // CAP + ep, groups)
    member = jnp.zeros((slots, count), jnp.float32)
    weight = jnp.zeros((slots, count), jnp.float32)
    loads[2].wait()
    loads[3].wait()
    for k in range(routing.shape[0]):
        named = routing[k:k + 1, :] == expert
        member = jnp.where(named, 1.0, member)
        weight = jnp.where(named, route_weight[k:k + 1, :], weight)
    earlier = lax.broadcasted_iota(jnp.int32, (count, count), 0) < lax.broadcasted_iota(jnp.int32, (count, count), 1)
    before = jnp.dot(member.astype(jnp.bfloat16), jnp.where(earlier, 1.0, 0.0).astype(jnp.bfloat16),
                     preferred_element_type=jnp.float32)
    placed = jnp.where(before == lax.rem(line, CAP).astype(jnp.float32), member, 0.0)
    weight = jnp.transpose(weight * placed)

    loads[0].wait()
    loads[1].wait()
    values = tokens[...].astype(jnp.float32)
    scale = lax.rsqrt(jnp.mean(values * values, axis=-1, keepdims=True) + norm_eps)
    normed = (values * scale * gain[...]).astype(jnp.bfloat16)
    sent = jnp.dot(placed.astype(jnp.bfloat16), normed, preferred_element_type=jnp.float32)
    outgoing[...] = sent.reshape(groups, CAP, width).astype(jnp.bfloat16)

    pl.semaphore_wait(barrier, groups + shares - 2)

    def dispatch(d):
        pltpu.make_async_remote_copy(
            src_ref=outgoing.at[d], dst_ref=incoming.at[d], send_sem=send_sem.at[0], recv_sem=recv_sem.at[0],
            device_id=(lax.rem(ep + d, groups), tp), device_id_type=MESH).start()
    each(1, groups, dispatch)
    incoming[0] = outgoing[0]

    loads[4].wait()
    loads[5].wait()
    loads[6].wait()
    others = pl.ds(1, groups - 1)
    pltpu.make_async_copy(incoming.at[others], incoming.at[others], recv_sem.at[0]).wait()

    x = incoming[...].astype(jnp.float32).reshape(slots, width).astype(jnp.bfloat16)
    gate_act = jnp.dot(x, gate[...], preferred_element_type=jnp.float32)
    up_act = jnp.dot(x, up[...], preferred_element_type=jnp.float32)
    hidden = (gate_act / (1.0 + jnp.exp(-gate_act)) * up_act).astype(jnp.bfloat16)

    def block_of(q, side):
        columns = pl.ds(pl.multiple_of((lax.rem(row + q, rows) * 2 + side) * part, part), part)
        return jnp.dot(hidden, down[:, columns], preferred_element_type=jnp.float32)

    def give(place, q, low, high):
        def to(step):
            target = far_first(step)

            def copy():
                d = lax.rem(ep - target + groups, groups)
                pltpu.make_async_remote_copy(
                    src_ref=partial.at[place * groups + d], dst_ref=arrived.at[place * groups + d],
                    send_sem=send_sem.at[1], recv_sem=recv_sem.at[1],
                    device_id=(target, toward(q)), device_id_type=MESH).start()
            if q == 0:
                pl.when(target != ep)(copy)
            else:
                copy()
        each(low, high, to)

    half = groups // 2

    for q in range(2, shares):
        block = block_of(q // 2, lax.rem(core + q, 2))
        partial[(q - 1) * groups:q * groups] = block.reshape(groups, CAP, part)
        give(q - 1, q, 0, half)

    lent[...] = block_of(0, 1 - core)
    lend = pltpu.make_async_remote_copy(
        src_ref=lent, dst_ref=borrowed, send_sem=send_sem.at[2], recv_sem=recv_sem.at[2],
        device_id=(ep, toward(1)), device_id_type=MESH)
    lend.start()
    block = block_of(0, core)
    for q in range(2, shares):
        give(q - 1, q, half, groups)
    lend.wait_recv()
    partial[0:groups] = (block + borrowed[...]).reshape(groups, CAP, part)
    give(0, 0, 0, groups)
    arrived[0] = partial[0]

    rest = pl.ds(1, groups * (shares - 1) - 1)
    pltpu.make_async_copy(arrived.at[rest], arrived.at[rest], recv_sem.at[1]).wait()
    total = arrived[0:groups]
    for q in range(1, shares - 1):
        total = total + arrived[q * groups:(q + 1) * groups]
    out = jnp.dot(weight, total.reshape(slots, part), precision=lax.Precision.HIGHEST,
                  preferred_element_type=jnp.float32)
    mixed[...] = out.astype(mixed.dtype)
    pltpu.make_async_copy(outgoing.at[others], outgoing.at[others], send_sem.at[0]).wait()
    pltpu.make_async_copy(partial.at[rest], partial.at[rest], send_sem.at[1]).wait()
    lend.wait_send()


def solution(mesh):
    groups, shares = mesh.shape["ep"], mesh.shape["tp"]

    def local(tokens, norm_gain, routing, route_weight, w_gate, w_up, w_down):
        count, width = tokens.shape
        part = width // shares
        vmem = pl.BlockSpec(memory_space=pltpu.VMEM)
        hbm = pl.BlockSpec(memory_space=pltpu.HBM)
        return pl.pallas_call(
            functools.partial(kernel, groups, shares),
            out_shape=jax.ShapeDtypeStruct((count, part), jnp.bfloat16),
            in_specs=[hbm] * 7,
            out_specs=vmem,
            scratch_shapes=[
                pltpu.VMEM((count, width), tokens.dtype),
                pltpu.VMEM((1, width), norm_gain.dtype),
                pltpu.VMEM(routing.shape[::-1], routing.dtype),
                pltpu.VMEM(route_weight.shape[::-1], route_weight.dtype),
                pltpu.VMEM(w_gate.shape[1:], jnp.bfloat16),
                pltpu.VMEM(w_up.shape[1:], jnp.bfloat16),
                pltpu.VMEM(w_down.shape[1:], jnp.bfloat16),
                pltpu.VMEM((groups, CAP, width), jnp.bfloat16),
                pltpu.VMEM((groups, CAP, width), jnp.bfloat16),
                pltpu.VMEM((groups * CAP, part), jnp.float32),
                pltpu.VMEM((groups * CAP, part), jnp.float32),
                pltpu.VMEM((groups * (shares - 1), CAP, part), jnp.float32),
                pltpu.VMEM((groups * (shares - 1), CAP, part), jnp.float32),
                pltpu.SemaphoreType.DMA((7,)),
                pltpu.SemaphoreType.DMA((3,)),
                pltpu.SemaphoreType.DMA((3,)),
            ],
            compiler_params=pltpu.CompilerParams(collective_id=0, has_side_effects=True,
                                                 vmem_limit_bytes=67043328),
            name="experts",
        )(tokens, norm_gain.reshape(1, width), routing.T, route_weight.T, w_gate, w_up, w_down)

    in_specs = (
        P("ep", None),
        P(),
        P("ep", None),
        P("ep", None),
        P("ep", None, "tp"),
        P("ep", None, "tp"),
        P("ep", "tp", None),
    )
    return jax.shard_map(local, mesh=mesh, in_specs=in_specs, out_specs=P("ep", "tp"), check_vma=False)
```

```python
import functools

import jax
import jax.numpy as jnp
from jax import lax
from jax.experimental import pallas as pl
from jax.experimental.pallas import tpu as pltpu
from jax.sharding import PartitionSpec as P

CAP = 8
MESH = pl.DeviceIdType.MESH

norm_eps = 1e-06


def each(low, high, step):
    if high - low <= 8:
        for index in range(low, high):
            step(index)
    else:
        lax.fori_loop(low, high, lambda index, carry: (step(index), carry)[1], 0)


def kernel(groups, shares, tokens_hbm, gain_hbm, routing_hbm, route_weight_hbm, gate_hbm, up_hbm, down_hbm, mixed,
           tokens, gain, routing, route_weight,
           gate, up, down, outgoing, incoming, lent, borrowed, partial, arrived, load_sem, send_sem, recv_sem):
    ep, tp = lax.axis_index("ep"), lax.axis_index("tp")
    width = tokens.shape[1]
    part = mixed.shape[1]
    slots = groups * CAP
    rows = shares // 2
    row, core = tp // 2, lax.rem(tp, 2)

    def toward(q):
        return lax.rem(row + q // 2, rows) * 2 + lax.rem(core + q % 2, 2)

    def far_first(step):
        return step + (1 - 2 * ep // groups) * (groups - 1 - 2 * step)

    pairs = ((tokens_hbm, tokens), (gain_hbm, gain), (routing_hbm, routing), (route_weight_hbm, route_weight),
             (gate_hbm.at[0], gate), (up_hbm.at[0], up), (down_hbm.at[0], down))
    loads = [pltpu.make_async_copy(source, target, load_sem.at[i]) for i, (source, target) in enumerate(pairs)]
    for load in loads:
        load.start()

    barrier = pltpu.get_barrier_semaphore()

    def greet(d):
        pl.semaphore_signal(barrier, inc=1, device_id=(lax.rem(ep + d, groups), tp), device_id_type=MESH)
    each(1, groups, greet)
    for q in range(1, shares):
        pl.semaphore_signal(barrier, inc=1, device_id=(ep, toward(q)), device_id_type=MESH)

    count = tokens.shape[0]
    line = lax.broadcasted_iota(jnp.int32, (slots, count), 0)
    expert = lax.rem(line // CAP + ep, groups)
    member = jnp.zeros((slots, count), jnp.float32)
    weight = jnp.zeros((slots, count), jnp.float32)
    loads[2].wait()
    loads[3].wait()
    for k in range(routing.shape[0]):
        named = routing[k:k + 1, :] == expert
        member = jnp.where(named, 1.0, member)
        weight = jnp.where(named, route_weight[k:k + 1, :], weight)
    earlier = lax.broadcasted_iota(jnp.int32, (count, count), 0) < lax.broadcasted_iota(jnp.int32, (count, count), 1)
    before = jnp.dot(member.astype(jnp.bfloat16), jnp.where(earlier, 1.0, 0.0).astype(jnp.bfloat16),
                     preferred_element_type=jnp.float32)
    placed = jnp.where(before == lax.rem(line, CAP).astype(jnp.float32), member, 0.0)
    weight = jnp.transpose(weight * placed)

    loads[0].wait()
    loads[1].wait()
    values = tokens[...].astype(jnp.float32)
    scale = lax.rsqrt(jnp.mean(values * values, axis=-1, keepdims=True) + norm_eps)
    normed = (values * scale * gain[...]).astype(jnp.bfloat16)
    sent = jnp.dot(placed.astype(jnp.bfloat16), normed, preferred_element_type=jnp.float32)
    outgoing[...] = sent.reshape(groups, CAP, width).astype(jnp.bfloat16)

    pl.semaphore_wait(barrier, groups + shares - 2)

    def dispatch(d):
        pltpu.make_async_remote_copy(
            src_ref=outgoing.at[d], dst_ref=incoming.at[d], send_sem=send_sem.at[0], recv_sem=recv_sem.at[0],
            device_id=(lax.rem(ep + d, groups), tp), device_id_type=MESH).start()
    each(1, groups, dispatch)
    incoming[0] = outgoing[0]

    loads[4].wait()
    loads[5].wait()
    loads[6].wait()
    others = pl.ds(1, groups - 1)
    pltpu.make_async_copy(incoming.at[others], incoming.at[others], recv_sem.at[0]).wait()

    x = incoming[...].astype(jnp.float32).reshape(slots, width).astype(jnp.bfloat16)
    gate_act = jnp.dot(x, gate[...], preferred_element_type=jnp.float32)
    up_act = jnp.dot(x, up[...], preferred_element_type=jnp.float32)
    hidden = (gate_act / (1.0 + jnp.exp(-gate_act)) * up_act).astype(jnp.bfloat16)

    def block_of(q, side):
        columns = pl.ds(pl.multiple_of((lax.rem(row + q, rows) * 2 + side) * part, part), part)
        return jnp.dot(hidden, down[:, columns], preferred_element_type=jnp.float32)

    def give(place, q, low, high):
        def to(step):
            target = far_first(step)

            def copy():
                d = lax.rem(ep - target + groups, groups)
                pltpu.make_async_remote_copy(
                    src_ref=partial.at[place * groups + d], dst_ref=arrived.at[place * groups + d],
                    send_sem=send_sem.at[1], recv_sem=recv_sem.at[3 if place == 0 else 1],
                    device_id=(target, toward(q)), device_id_type=MESH).start()
            if q == 0:
                pl.when(target != ep)(copy)
            else:
                copy()
        each(low, high, to)

    half = groups // 2

    for q in range(2, shares):
        block = block_of(q // 2, lax.rem(core + q, 2))
        partial[(q - 1) * groups:q * groups] = block.reshape(groups, CAP, part)
        give(q - 1, q, 0, half)

    lent[...] = block_of(0, 1 - core)
    lend = pltpu.make_async_remote_copy(
        src_ref=lent, dst_ref=borrowed, send_sem=send_sem.at[2], recv_sem=recv_sem.at[2],
        device_id=(ep, toward(1)), device_id_type=MESH)
    lend.start()
    block = block_of(0, core)
    for q in range(2, shares):
        give(q - 1, q, half, groups)
    lend.wait_recv()
    partial[0:groups] = (block + borrowed[...]).reshape(groups, CAP, part)
    give(0, 0, 0, groups)
    arrived[0] = partial[0]

    def mix(blocks):
        return jnp.dot(weight, blocks.reshape(slots, part), precision=lax.Precision.HIGHEST,
                       preferred_element_type=jnp.float32)

    rest = pl.ds(1, groups * (shares - 1) - 1)
    far = pl.ds(groups, groups * (shares - 2))
    pltpu.make_async_copy(arrived.at[others], arrived.at[others], recv_sem.at[3]).wait()
    out = mix(arrived[0:groups])
    pltpu.make_async_copy(arrived.at[far], arrived.at[far], recv_sem.at[1]).wait()
    total = arrived[groups:2 * groups]
    for q in range(2, shares - 1):
        total = total + arrived[q * groups:(q + 1) * groups]
    out = out + mix(total)
    mixed[...] = out.astype(mixed.dtype)
    pltpu.make_async_copy(outgoing.at[others], outgoing.at[others], send_sem.at[0]).wait()
    pltpu.make_async_copy(partial.at[rest], partial.at[rest], send_sem.at[1]).wait()
    lend.wait_send()


def solution(mesh):
    groups, shares = mesh.shape["ep"], mesh.shape["tp"]

    def local(tokens, norm_gain, routing, route_weight, w_gate, w_up, w_down):
        count, width = tokens.shape
        part = width // shares
        vmem = pl.BlockSpec(memory_space=pltpu.VMEM)
        hbm = pl.BlockSpec(memory_space=pltpu.HBM)
        return pl.pallas_call(
            functools.partial(kernel, groups, shares),
            out_shape=jax.ShapeDtypeStruct((count, part), jnp.bfloat16),
            in_specs=[hbm] * 7,
            out_specs=vmem,
            scratch_shapes=[
                pltpu.VMEM((count, width), tokens.dtype),
                pltpu.VMEM((1, width), norm_gain.dtype),
                pltpu.VMEM(routing.shape[::-1], routing.dtype),
                pltpu.VMEM(route_weight.shape[::-1], route_weight.dtype),
                pltpu.VMEM(w_gate.shape[1:], jnp.bfloat16),
                pltpu.VMEM(w_up.shape[1:], jnp.bfloat16),
                pltpu.VMEM(w_down.shape[1:], jnp.bfloat16),
                pltpu.VMEM((groups, CAP, width), jnp.bfloat16),
                pltpu.VMEM((groups, CAP, width), jnp.bfloat16),
                pltpu.VMEM((groups * CAP, part), jnp.float32),
                pltpu.VMEM((groups * CAP, part), jnp.float32),
                pltpu.VMEM((groups * (shares - 1), CAP, part), jnp.float32),
                pltpu.VMEM((groups * (shares - 1), CAP, part), jnp.float32),
                pltpu.SemaphoreType.DMA((7,)),
                pltpu.SemaphoreType.DMA((4,)),
                pltpu.SemaphoreType.DMA((4,)),
            ],
            compiler_params=pltpu.CompilerParams(collective_id=0, has_side_effects=True,
                                                 vmem_limit_bytes=67043328),
            name="experts",
        )(tokens, norm_gain.reshape(1, width), routing.T, route_weight.T, w_gate, w_up, w_down)

    in_specs = (
        P("ep", None),
        P(),
        P("ep", None),
        P("ep", None),
        P("ep", None, "tp"),
        P("ep", None, "tp"),
        P("ep", "tp", None),
    )
    return jax.shard_map(local, mesh=mesh, in_specs=in_specs, out_specs=P("ep", "tp"), check_vma=False)
```
